32 devices in a mesh: kv: 8 (over z, x), tp: 4 (over y, core).
Axes of the slice: x: 2, y: 2, z: 4, core: 2. Of those that a mesh axis runs over, the one named last changes fastest.
Arguments:
- tokens: bfloat16 [256, 2048], P('kv', 'tp'), may hold values from -60 to 60, as said below
- memory: float32 [256, 8, 128, 128], P('kv', 'tp'), may hold values from -0.6 to 0.6
- normalizer: float32 [256, 8, 128], P('kv', 'tp'), may hold values from -0.6 to 0.6
- stabilizer: float32 [256, 8], P('kv', 'tp'), may hold values from -4 to 4
- norm_gain: float32 [2048], replicated, may hold values from 0.1 to 1.9
- query_weight: bfloat16 [2048, 1024], P(None, 'tp'), may hold values from -0.125 to 0.125
- key_weight: bfloat16 [2048, 1024], P(None, 'tp'), may hold values from -0.125 to 0.125
- value_weight: bfloat16 [2048, 1024], P(None, 'tp'), may hold values from -0.125 to 0.125
- outgate_weight: bfloat16 [2048, 1024], P(None, 'tp'), may hold values from -0.125 to 0.125
- input_gate_weight: bfloat16 [2048, 8], replicated, may hold values from -0.125 to 0.125
- forget_gate_weight: bfloat16 [2048, 8], replicated, may hold values from -0.125 to 0.125
- forget_bias: float32 [8], replicated, may hold values from -1 to 5
- memory_gain: float32 [1024], P('tp'), may hold values from 0.1 to 1.9
- proj_weight: bfloat16 [1024, 2048], P(None, 'tp'), may hold values from -0.1875 to 0.1875
- ffn_gain: float32 [2048], P('tp'), may hold values from 0.1 to 1.9
- up_weight: bfloat16 [2048, 8192], P('tp', 'kv'), may hold values from -0.125 to 0.125
- down_weight: bfloat16 [8192, 2048], P('kv', 'tp'), may hold values from -0.0625 to 0.0625
Outputs:
- layer_out: bfloat16 [256, 2048], P('kv', 'tp')
- memory_new: float32 [256, 8, 128, 128], P('kv', 'tp')
- normalizer_new: float32 [256, 8, 128], P('kv', 'tp')
- stabilizer_new: float32 [256, 8], P('kv', 'tp')
The draws below stay inside these ranges and needn't reach their ends.
Inputs may be any that keep to these rules, and one draw needn't show every extreme that they name: `tokens`: activations whose feature blocks and rows differ in scale.
All inputs are finite; a program needn't handle non-finite values.
Results may differ from the reference program's by a relative error of at most 0.0095.
Values may be sent and summed in bfloat16 or wider, within the bound.
No kernel may reach another device: no remote copies, remote signals or barrier semaphores. Data moves between devices by JAX's collectives and lax.ppermute only.
A program may use at most 64 MiB of HBM per device.

```python
import math
import jax
import jax.numpy as jnp
from jax import lax

D = 2048
H = 8
DK = 128
DV = 128
FF = 8192
SEQS = 256


def draw_tokens(key, part):
    key_base = jax.random.fold_in(key, 11)
    key_cols = jax.random.fold_in(key, 12)
    key_rows = jax.random.fold_in(key, 13)
    column = jnp.arange(D, dtype=jnp.float32) / (D - 1)
    col_scale = jnp.exp(column * math.log(3.0)) / 1.7 * jnp.exp(jax.random.uniform(key_cols, (D,), jnp.float32, math.log(0.6), math.log(1.6)))
    base = jnp.clip(jax.random.normal(key_base, (SEQS, D), jnp.float32), -4.0, 4.0)
    row_scale = jnp.exp(jax.random.uniform(key_rows, (SEQS, 1), jnp.float32, math.log(0.3), math.log(3.0)))
    return (base * row_scale * col_scale[None, :]).astype(jnp.bfloat16)


def shard_levels(own_key, extent, pieces, low, largest):
    factor_of = 1.0
    for position, blocks in pieces:
        steps = jax.random.uniform(jax.random.fold_in(jax.random.fold_in(own_key, 6), position), (blocks,), jnp.float32, low / len(pieces), largest / len(pieces))
        factor_of = factor_of * jnp.repeat(jnp.exp(steps), extent[position] // blocks).reshape((-1,) + (1,) * (len(extent) - 1 - position))
    return factor_of


def scatter_about(key, extent, width, most, shards=(), kind=jnp.bfloat16):
    values = width * jax.random.normal(key, extent, jnp.float32)
    if shards:
        values = values * shard_levels(key, extent, shards, -0.22, 0.18)
    return jnp.clip(values, -most, most).astype(kind)


def setup_inputs(seed: int = 0) -> dict:
    key_list = jax.random.split(jax.random.key(seed), 18)
    return {
        "tokens": draw_tokens(jax.random.fold_in(key_list[17], 71), 0),
        "memory": scatter_about(key_list[1], (SEQS, H, DV, DK), 0.1, 0.6, ((0, 8), (1, 4)), jnp.float32),
        "normalizer": scatter_about(key_list[2], (SEQS, H, DK), 0.1, 0.6, ((0, 8), (1, 4)), jnp.float32),
        "stabilizer": scatter_about(key_list[3], (SEQS, H), 1.0, 4.0, ((0, 8), (1, 4)), jnp.float32),
        "norm_gain": jnp.clip(1.0 + 0.18 * jax.random.normal(key_list[4], (D,), jnp.float32), 0.1, 1.9),
        "query_weight": scatter_about(key_list[5], (D, H * DK), D ** -0.5, 0.125, ((1, 4),)),
        "key_weight": scatter_about(key_list[6], (D, H * DK), D ** -0.5, 0.125, ((1, 4),)),
        "value_weight": scatter_about(key_list[7], (D, H * DV), D ** -0.5, 0.125, ((1, 4),)),
        "outgate_weight": scatter_about(key_list[8], (D, H * DV), D ** -0.5, 0.125, ((1, 4),)),
        "input_gate_weight": scatter_about(key_list[9], (D, H), D ** -0.5, 0.125),
        "forget_gate_weight": scatter_about(key_list[10], (D, H), D ** -0.5, 0.125),
        "forget_bias": jnp.clip(jax.random.uniform(key_list[11], (H,), jnp.float32, -1.0, 5.0), -1.0, 5.0),
        "memory_gain": jnp.clip(1.0 + 0.18 * jax.random.normal(key_list[12], (H * DV,), jnp.float32), 0.1, 1.9),
        "proj_weight": scatter_about(key_list[13], (H * DV, D), (H * DV) ** -0.5, 0.1875, ((1, 4),)),
        "ffn_gain": jnp.clip(1.0 + 0.18 * jax.random.normal(key_list[14], (D,), jnp.float32), 0.1, 1.9),
        "up_weight": scatter_about(key_list[15], (D, FF), D ** -0.5, 0.125, ((0, 4), (1, 8))),
        "down_weight": scatter_about(key_list[16], (FF, D), FF ** -0.5, 0.0625, ((0, 8), (1, 4))),
    }


EPS = 1e-06

def reference(tokens, memory, normalizer, stabilizer, norm_gain, query_weight, key_weight, value_weight, outgate_weight, input_gate_weight, forget_gate_weight, forget_bias, memory_gain, proj_weight, ffn_gain, up_weight, down_weight):
    rows_f = tokens.astype(jnp.float32)
    scale_one = lax.rsqrt(lax.optimization_barrier(jnp.mean(rows_f * rows_f, axis=-1, keepdims=True)) + EPS)
    normed = (rows_f * scale_one * norm_gain).astype(jnp.bfloat16)
    count = tokens.shape[0]
    query = jnp.dot(normed, query_weight, preferred_element_type=jnp.float32).astype(jnp.bfloat16)
    keys = jnp.dot(normed, key_weight, preferred_element_type=jnp.float32).astype(jnp.bfloat16)
    values = jnp.dot(normed, value_weight, preferred_element_type=jnp.float32).astype(jnp.bfloat16)
    gate_out = jnp.dot(normed, outgate_weight, preferred_element_type=jnp.float32).astype(jnp.bfloat16)
    input_log = jnp.dot(normed, input_gate_weight, preferred_element_type=jnp.float32)
    forget_log = jax.nn.log_sigmoid(jnp.dot(normed, forget_gate_weight, preferred_element_type=jnp.float32) + forget_bias)
    query_f = query.astype(jnp.float32).reshape(count, H, DK)
    keys_f = keys.astype(jnp.float32).reshape(count, H, DK) * DK ** (-0.5)
    values_f = values.astype(jnp.float32).reshape(count, H, DV)
    stab_new = jnp.maximum(forget_log + stabilizer, input_log)
    keep = jnp.exp(forget_log + stabilizer - stab_new)
    admit = jnp.exp(input_log - stab_new)
    memory_new = keep[..., None, None] * memory + admit[..., None, None] * values_f[..., :, None] * keys_f[..., None, :]
    normalizer_new = keep[..., None] * normalizer + admit[..., None] * keys_f
    numer = jnp.einsum('bhed,bhd->bhe', memory_new, query_f, precision=lax.Precision.HIGHEST)
    denom = lax.optimization_barrier(jnp.sum(normalizer_new * query_f, axis=-1))
    cell = numer / jnp.maximum(jnp.abs(denom), 1.0)[..., None]
    mixed = (cell.reshape(count, H * DV) * memory_gain * jax.nn.sigmoid(gate_out.astype(jnp.float32))).astype(jnp.bfloat16)
    second = (rows_f + jnp.dot(mixed, proj_weight, preferred_element_type=jnp.float32)).astype(jnp.bfloat16)
    second_f = second.astype(jnp.float32)
    scale_two = lax.rsqrt(lax.optimization_barrier(jnp.mean(second_f * second_f, axis=-1, keepdims=True)) + EPS)
    scaled = (second_f * ffn_gain).astype(jnp.bfloat16)
    preact = jnp.dot(scaled, up_weight, preferred_element_type=jnp.float32)
    hidden = jnp.square(jax.nn.relu(preact * scale_two)).astype(jnp.bfloat16)
    layer_out = (second_f + jnp.dot(hidden, down_weight, preferred_element_type=jnp.float32)).astype(jnp.bfloat16)
    return (layer_out, memory_new, normalizer_new, stab_new)
```

```python
import jax
import jax.numpy as jnp
from jax import lax
from jax.sharding import PartitionSpec as P

D = 2048
DK = 128
DV = 128


EPS = 1e-06


def sum_over(partial, axis, dim):
    parts = lax.axis_size(axis)
    sent = partial.astype(jnp.bfloat16)
    if dim == 1:
        sent = sent.reshape(sent.shape[0], parts, -1).transpose(1, 0, 2)
    else:
        sent = sent.reshape(parts, -1, sent.shape[1])
    got = lax.all_to_all(sent, axis, 0, 0, tiled=True)
    return jnp.sum(got.astype(jnp.float32), axis=0)


def per_device(
    tokens,
    memory,
    normalizer,
    stabilizer,
    norm_gain,
    query_weight,
    key_weight,
    value_weight,
    outgate_weight,
    input_gate_weight,
    forget_gate_weight,
    forget_bias,
    memory_gain,
    proj_weight,
    ffn_gain,
    up_weight,
    down_weight,
):
    own_rows = tokens.shape[0]
    heads_here = memory.shape[1]
    first_head = lax.axis_index("tp") * heads_here
    full_rows = lax.all_gather(tokens, "tp", axis=1, tiled=True)
    rows_f = full_rows.astype(jnp.float32)
    scale_one = lax.rsqrt(jnp.mean(rows_f * rows_f, axis=-1, keepdims=True) + EPS)
    normed = (rows_f * scale_one * norm_gain).astype(jnp.bfloat16)
    query = jnp.dot(normed, query_weight, preferred_element_type=jnp.float32).astype(jnp.bfloat16)
    keys = jnp.dot(normed, key_weight, preferred_element_type=jnp.float32).astype(jnp.bfloat16)
    values = jnp.dot(normed, value_weight, preferred_element_type=jnp.float32).astype(jnp.bfloat16)
    gate_out = jnp.dot(normed, outgate_weight, preferred_element_type=jnp.float32).astype(
        jnp.bfloat16
    )
    input_cols = lax.dynamic_slice_in_dim(input_gate_weight, first_head, heads_here, 1)
    forget_cols = lax.dynamic_slice_in_dim(forget_gate_weight, first_head, heads_here, 1)
    bias_here = lax.dynamic_slice_in_dim(forget_bias, first_head, heads_here, 0)
    input_log = jnp.dot(normed, input_cols, preferred_element_type=jnp.float32)
    forget_log = jax.nn.log_sigmoid(
        jnp.dot(normed, forget_cols, preferred_element_type=jnp.float32) + bias_here
    )
    query_f = query.astype(jnp.float32).reshape(own_rows, heads_here, DK)
    keys_f = keys.astype(jnp.float32).reshape(own_rows, heads_here, DK) * DK ** (-0.5)
    values_f = values.astype(jnp.float32).reshape(own_rows, heads_here, DV)
    stab_new = jnp.maximum(forget_log + stabilizer, input_log)
    keep = jnp.exp(forget_log + stabilizer - stab_new)
    admit = jnp.exp(input_log - stab_new)
    memory_new = (
        keep[..., None, None] * memory
        + admit[..., None, None] * values_f[..., :, None] * keys_f[..., None, :]
    )
    normalizer_new = keep[..., None] * normalizer + admit[..., None] * keys_f
    numer = jnp.einsum("bhed,bhd->bhe", memory_new, query_f, precision=lax.Precision.HIGHEST)
    denom = jnp.sum(normalizer_new * query_f, axis=-1)
    cell = numer / jnp.maximum(jnp.abs(denom), 1.0)[..., None]
    mixed = (
        cell.reshape(own_rows, heads_here * DV)
        * memory_gain
        * jax.nn.sigmoid(gate_out.astype(jnp.float32))
    ).astype(jnp.bfloat16)
    projected = jnp.dot(
        lax.all_gather(mixed, "tp", axis=1, tiled=True),
        proj_weight,
        preferred_element_type=jnp.float32,
    )
    second = (tokens.astype(jnp.float32) + projected).astype(jnp.bfloat16)
    groups = lax.axis_size("kv")
    all_rows = lax.all_to_all(
        jnp.broadcast_to(second, (groups,) + second.shape), "kv", 0, 0, tiled=True
    ).reshape(groups * own_rows, second.shape[1])
    all_f = all_rows.astype(jnp.float32)
    square_sum = jnp.sum(all_f * all_f, axis=-1)
    scaled = (all_f * ffn_gain).astype(jnp.bfloat16)
    preact = jnp.dot(scaled, up_weight, preferred_element_type=jnp.float32)
    share = sum_over(preact, "tp", 1)
    square_sum = lax.psum(square_sum, "tp")
    scale_two = lax.rsqrt(square_sum / D + EPS)
    partial_hidden = jnp.square(jax.nn.relu(share * scale_two[:, None])).astype(jnp.bfloat16)
    hidden = lax.all_gather(partial_hidden, "tp", axis=1, tiled=True)
    summed = sum_over(jnp.dot(hidden, down_weight, preferred_element_type=jnp.float32), "kv", 0)
    layer_out = (second.astype(jnp.float32) + summed).astype(jnp.bfloat16)
    return (layer_out, memory_new, normalizer_new, stab_new)


def solution(mesh):
    placed = (
        P("kv", "tp"),
        P("kv", "tp", None, None),
        P("kv", "tp", None),
        P("kv", "tp"),
        P(),
        P(None, "tp"),
        P(None, "tp"),
        P(None, "tp"),
        P(None, "tp"),
        P(),
        P(),
        P(),
        P("tp"),
        P(None, "tp"),
        P("tp"),
        P("tp", "kv"),
        P("kv", "tp"),
    )
    return jax.shard_map(
        per_device,
        mesh=mesh,
        in_specs=placed,
        out_specs=(P("kv", "tp"), P("kv", "tp", None, None), P("kv", "tp", None), P("kv", "tp")),
        check_vma=False,
    )
```

```python
import functools
import jax
import jax.numpy as jnp
from jax import lax
from jax.experimental import pallas as pl
from jax.experimental.pallas import tpu as pltpu
from jax.sharding import PartitionSpec as P

D = 2048
DK = 128
DV = 128


EPS = 1e-06


GROUP = 16


def cell_kernel(
    heads,
    *refs,
):
    blocks = lax.axis_size("tp")
    cell_body(heads, refs[:blocks], *refs[blocks:])


def cell_body(
    heads,
    rows_refs,
    gain_ref,
    query_ref,
    key_ref,
    value_ref,
    outgate_ref,
    input_ref,
    forget_ref,
    bias_ref,
    stabilizer_ref,
    normalizer_ref,
    memory_ref,
    memory_gain_ref,
    mixed_ref,
    normalizer_new_ref,
    stab_new_ref,
    keep_ref,
    admit_ref,
    keys_out_ref,
    values_out_ref,
):
    bf, f32 = jnp.bfloat16, jnp.float32
    first_head = lax.axis_index("tp") * heads
    me = lax.axis_index("tp")
    width = rows_refs[0].shape[1]
    squares = [jnp.square(ref[...].astype(f32)) for ref in rows_refs]
    squares = [jnp.sum(s, axis=-1, keepdims=True) for s in squares]
    scale_one = lax.rsqrt(sum(squares) / (width * len(squares)) + EPS)
    transposed = (((1,), (1,)), ((), ()))
    sums = [0.0] * 6
    for b, ref in enumerate(rows_refs):
        at = pl.ds(pl.multiple_of((me ^ b) * width, width), width)
        normed = (ref[...].astype(f32) * scale_one * gain_ref[:, at]).astype(bf)
        for n, w in enumerate((input_ref, forget_ref)):
            sums[n] += lax.dot_general(normed, w[:, at], transposed, preferred_element_type=f32)
        for n, w in enumerate((key_ref, query_ref, value_ref, outgate_ref)):
            sums[2 + n] += jnp.dot(normed, w[at, :], preferred_element_type=f32)
    input_all = sums[0]
    forget_all = jax.nn.log_sigmoid(sums[1] + bias_ref[...])
    keys, query, values, gate_out = (s.astype(bf) for s in sums[2:])
    keys_out_ref[...] = keys
    values_out_ref[...] = values
    lane = lax.broadcasted_iota(jnp.int32, input_all.shape, 1)
    count = rows_refs[0].shape[0]
    own = lax.broadcasted_iota(jnp.int32, keep_ref.shape, 1)
    diagonal = lax.broadcasted_iota(jnp.int32, (count, count), 0) == lax.broadcasted_iota(
        jnp.int32, (count, count), 1
    )
    keep_all, admit_all = (jnp.zeros(keep_ref.shape, f32) for _ in range(2))
    for h in range(heads):
        chosen = lane == first_head + h
        input_log = jnp.sum(jnp.where(chosen, input_all, 0.0), axis=1, keepdims=True)
        forget_log = jnp.sum(jnp.where(chosen, forget_all, 0.0), axis=1, keepdims=True)
        before = jnp.where(diagonal, stabilizer_ref[h : h + 1, :], 0.0)
        decayed = forget_log + jnp.sum(before, axis=1, keepdims=True)
        stab = jnp.maximum(decayed, input_log)
        keep = jnp.exp(decayed - stab)
        admit = jnp.exp(input_log - stab)
        stab_new_ref[h : h + 1, :] = jnp.sum(jnp.where(diagonal, stab, 0.0), axis=0, keepdims=True)
        keep_all = jnp.where(own == h, keep, keep_all)
        admit_all = jnp.where(own == h, admit, admit_all)
        cols = slice(h * DK, (h + 1) * DK)
        vcols = slice(h * DV, (h + 1) * DV)
        keys_f = keys[:, cols].astype(f32) * DK ** (-0.5)
        query_f = query[:, cols].astype(f32)
        normalizer_new = keep * normalizer_ref[:, h, :] + admit * keys_f
        normalizer_new_ref[:, h, :] = normalizer_new
        denom = jnp.sum(normalizer_new * query_f, axis=-1, keepdims=True)
        match = jnp.sum(keys_f * query_f, axis=-1, keepdims=True)
        groups = []
        for r in range(0, count, GROUP):
            some = query[r : r + GROUP, cols]
            place = lax.broadcasted_iota(jnp.int32, (GROUP, DV), 0)
            recalled = jnp.zeros((GROUP, DV), f32)
            for j in range(GROUP):
                stored = memory_ref[r + j, h].astype(bf)
                one = lax.dot_general(some, stored, transposed, preferred_element_type=f32)
                recalled = jnp.where(place == j, one, recalled)
            groups.append(recalled)
        recalled = jnp.concatenate(groups, axis=0)
        numer = keep * recalled + (admit * match) * values[:, vcols].astype(f32)
        cell = numer / jnp.maximum(jnp.abs(denom), 1.0)
        gate = jax.nn.sigmoid(gate_out[:, vcols].astype(f32))
        mixed_ref[:, vcols] = (cell * memory_gain_ref[:, vcols] * gate).astype(bf)
    keep_ref[...] = keep_all
    admit_ref[...] = admit_all


def fetch_kernel(count, *refs):
    copies = [
        pltpu.make_async_copy(refs[i], refs[count + i], refs[2 * count].at[i]) for i in range(count)
    ]
    for copy in copies:
        copy.start()
    for copy in copies:
        copy.wait()


def fetch(*args):
    args = [pltpu.with_memory_space_constraint(a, pltpu.HBM) for a in args]
    return pl.pallas_call(
        functools.partial(fetch_kernel, len(args)),
        out_shape=[pltpu.VMEM(a.shape, a.dtype) for a in args],
        in_specs=[pl.BlockSpec(memory_space=pltpu.HBM)] * len(args),
        out_specs=[pl.BlockSpec(memory_space=pltpu.VMEM)] * len(args),
        scratch_shapes=[pltpu.SemaphoreType.DMA((len(args),))],
        compiler_params=pltpu.CompilerParams(vmem_limit_bytes=2**20),
        cost_estimate=pl.CostEstimate(flops=10**9, bytes_accessed=9 * 2**20, transcendentals=0),
        name="fetch",
    )(*args)


def run_cell(blocks, heads, *args):
    own, f32 = blocks[0].shape[0], jnp.float32
    args = [pltpu.with_memory_space_constraint(a, pltpu.VMEM) for a in args]
    shapes = [
        ((own, heads * DV), jnp.bfloat16),
        ((own, heads, DK), f32),
        ((heads, own), f32),
        ((own, heads), f32),
        ((own, heads), f32),
        ((own, heads * DK), jnp.bfloat16),
        ((own, heads * DV), jnp.bfloat16),
    ]
    in_vmem = pl.BlockSpec(memory_space=pltpu.VMEM)
    return pl.pallas_call(
        functools.partial(cell_kernel, heads),
        out_shape=[jax.ShapeDtypeStruct(*s) for s in shapes],
        in_specs=[in_vmem] * (len(blocks) + len(args)),
        out_specs=[in_vmem] * len(shapes),
        compiler_params=pltpu.CompilerParams(vmem_limit_bytes=8 * 2**20),
        cost_estimate=pl.CostEstimate(flops=10**9, bytes_accessed=9 * 2**20, transcendentals=0),
        name="cell",
    )(*blocks, *args)


def swap(array, bit):
    pairs = [(i, i ^ bit) for i in range(lax.axis_size("tp"))]
    return lax.ppermute(array, "tp", pairs)


def per_device(
    tokens,
    memory,
    normalizer,
    stabilizer,
    norm_gain,
    query_weight,
    key_weight,
    value_weight,
    outgate_weight,
    input_gate_weight,
    forget_gate_weight,
    forget_bias,
    memory_gain,
    proj_weight,
    ffn_gain,
    up_weight,
    down_weight,
):
    own_rows = tokens.shape[0]
    heads_here = memory.shape[1]
    blocks = [tokens] + [swap(tokens, b) for b in reversed(range(1, lax.axis_size("tp")))][::-1]
    held = fetch(
        norm_gain.reshape(1, -1),
        query_weight,
        key_weight,
        value_weight,
        outgate_weight,
        input_gate_weight.T,
        forget_gate_weight.T,
        forget_bias.reshape(1, -1),
        stabilizer.T,
        normalizer,
        memory,
        memory_gain.reshape(1, -1),
    )
    mixed, normalizer_new, stab_new, keep, admit, keys, values = run_cell(blocks, heads_here, *held)
    stab_new = stab_new.T
    projected = jnp.dot(
        lax.all_gather(mixed, "tp", axis=1, tiled=True),
        proj_weight,
        preferred_element_type=jnp.float32,
    )
    second = (tokens.astype(jnp.float32) + projected).astype(jnp.bfloat16)
    second, keep, admit, keys, values = lax.optimization_barrier(
        (second, keep, admit, keys, values)
    )
    keys_f = keys.astype(jnp.float32).reshape(own_rows, heads_here, DK) * DK ** (-0.5)
    values_f = values.astype(jnp.float32).reshape(own_rows, heads_here, DV)
    memory_new = (
        keep[..., None, None] * memory
        + admit[..., None, None] * values_f[..., :, None] * keys_f[..., None, :]
    )
    groups = lax.axis_size("kv")
    all_rows = lax.all_to_all(
        jnp.broadcast_to(second, (groups,) + second.shape), "kv", 0, 0, tiled=True
    ).reshape(groups * own_rows, second.shape[1])
    scaled = (all_rows.astype(jnp.float32) * ffn_gain).astype(jnp.bfloat16)
    half = up_weight.shape[1] // 2
    side = lax.axis_index("tp") % 2
    mine, theirs = side * half, (1 - side) * half
    up_mine = lax.dynamic_slice_in_dim(up_weight, mine, half, 1)
    up_theirs = lax.dynamic_slice_in_dim(up_weight, theirs, half, 1)
    away = jnp.dot(scaled, up_theirs, preferred_element_type=jnp.float32).astype(jnp.bfloat16)
    came = swap(away, 1)
    preact = jnp.dot(scaled, up_mine, preferred_element_type=jnp.float32) + came.astype(jnp.float32)
    second_f = second.astype(jnp.float32)
    square_sum = jnp.sum(second_f * second_f, axis=-1, keepdims=True)
    square_sum = square_sum + swap(square_sum, 1)
    bit = 2
    while bit < lax.axis_size("tp"):
        sent = preact.astype(jnp.bfloat16)
        preact = sent.astype(jnp.float32) + swap(sent, bit).astype(jnp.float32)
        square_sum = square_sum + swap(square_sum, bit)
        bit *= 2
    hidden = jnp.square(jax.nn.relu(preact)).astype(jnp.bfloat16)
    other = swap(hidden, 1)
    down_mine = lax.dynamic_slice_in_dim(down_weight, mine, half, 0)
    down_theirs = lax.dynamic_slice_in_dim(down_weight, theirs, half, 0)
    partial = jnp.dot(hidden, down_mine, preferred_element_type=jnp.float32)
    partial = partial + jnp.dot(other, down_theirs, preferred_element_type=jnp.float32)
    sent = partial.astype(jnp.bfloat16).reshape(groups, own_rows, -1)
    got = lax.all_to_all(sent, "kv", 0, 0, tiled=True)
    summed = jnp.sum(got.astype(jnp.float32), axis=0)
    scale_two = lax.rsqrt(square_sum / D + EPS)
    layer_out = (second_f + summed * (scale_two * scale_two)).astype(jnp.bfloat16)
    return (layer_out, memory_new, normalizer_new, stab_new)


def solution(mesh):
    placed = (
        P("kv", "tp"),
        P("kv", "tp", None, None),
        P("kv", "tp", None),
        P("kv", "tp"),
        P(),
        P(None, "tp"),
        P(None, "tp"),
        P(None, "tp"),
        P(None, "tp"),
        P(),
        P(),
        P(),
        P("tp"),
        P(None, "tp"),
        P("tp"),
        P("tp", "kv"),
        P("kv", "tp"),
    )
    return jax.shard_map(
        per_device,
        mesh=mesh,
        in_specs=placed,
        out_specs=(P("kv", "tp"), P("kv", "tp", None, None), P("kv", "tp", None), P("kv", "tp")),
        check_vma=False,
    )
```

```python
import functools
import jax
import jax.numpy as jnp
from jax import lax
from jax.experimental import pallas as pl
from jax.experimental.pallas import tpu as pltpu
from jax.sharding import PartitionSpec as P

D = 2048
DK = 128
DV = 128


EPS = 1e-06


GROUP = 16
CHUNKS = 2


def cell_kernel(
    heads,
    *refs,
):
    blocks = lax.axis_size("tp")
    cell_body(heads, refs[:blocks], *refs[blocks:])


def cell_body(
    heads,
    rows_refs,
    gain_ref,
    query_ref,
    key_ref,
    value_ref,
    outgate_ref,
    input_ref,
    forget_ref,
    bias_ref,
    stabilizer_ref,
    normalizer_ref,
    memory_ref,
    memory_gain_ref,
    mixed_ref,
    normalizer_new_ref,
    stab_new_ref,
    keep_ref,
    admit_ref,
    keys_out_ref,
    values_out_ref,
):
    bf, f32 = jnp.bfloat16, jnp.float32
    first_head = lax.axis_index("tp") * heads
    me = lax.axis_index("tp")
    width = rows_refs[0].shape[1]
    squares = [jnp.square(ref[...].astype(f32)) for ref in rows_refs]
    squares = [jnp.sum(s, axis=-1, keepdims=True) for s in squares]
    scale_one = lax.rsqrt(sum(squares) / (width * len(squares)) + EPS)
    transposed = (((1,), (1,)), ((), ()))
    sums = [0.0] * 6
    for b, ref in enumerate(rows_refs):
        at = pl.ds(pl.multiple_of((me ^ b) * width, width), width)
        normed = (ref[...].astype(f32) * scale_one * gain_ref[:, at]).astype(bf)
        for n, w in enumerate((input_ref, forget_ref)):
            sums[n] += lax.dot_general(normed, w[:, at], transposed, preferred_element_type=f32)
        for n, w in enumerate((key_ref, query_ref, value_ref, outgate_ref)):
            sums[2 + n] += jnp.dot(normed, w[at, :], preferred_element_type=f32)
    input_all = sums[0]
    forget_all = jax.nn.log_sigmoid(sums[1] + bias_ref[...])
    keys, query, values, gate_out = (s.astype(bf) for s in sums[2:])
    keys_out_ref[...] = keys
    values_out_ref[...] = values
    lane = lax.broadcasted_iota(jnp.int32, input_all.shape, 1)
    count = rows_refs[0].shape[0]
    own = lax.broadcasted_iota(jnp.int32, keep_ref.shape, 1)
    diagonal = lax.broadcasted_iota(jnp.int32, (count, count), 0) == lax.broadcasted_iota(
        jnp.int32, (count, count), 1
    )
    keep_all, admit_all = (jnp.zeros(keep_ref.shape, f32) for _ in range(2))
    for h in range(heads):
        chosen = lane == first_head + h
        input_log = jnp.sum(jnp.where(chosen, input_all, 0.0), axis=1, keepdims=True)
        forget_log = jnp.sum(jnp.where(chosen, forget_all, 0.0), axis=1, keepdims=True)
        before = jnp.where(diagonal, stabilizer_ref[h : h + 1, :], 0.0)
        decayed = forget_log + jnp.sum(before, axis=1, keepdims=True)
        stab = jnp.maximum(decayed, input_log)
        keep = jnp.exp(decayed - stab)
        admit = jnp.exp(input_log - stab)
        stab_new_ref[h : h + 1, :] = jnp.sum(jnp.where(diagonal, stab, 0.0), axis=0, keepdims=True)
        keep_all = jnp.where(own == h, keep, keep_all)
        admit_all = jnp.where(own == h, admit, admit_all)
        cols = slice(h * DK, (h + 1) * DK)
        vcols = slice(h * DV, (h + 1) * DV)
        keys_f = keys[:, cols].astype(f32) * DK ** (-0.5)
        query_f = query[:, cols].astype(f32)
        normalizer_new = keep * normalizer_ref[:, h, :] + admit * keys_f
        normalizer_new_ref[:, h, :] = normalizer_new
        denom = jnp.sum(normalizer_new * query_f, axis=-1, keepdims=True)
        match = jnp.sum(keys_f * query_f, axis=-1, keepdims=True)
        groups = []
        for r in range(0, count, GROUP):
            some = query[r : r + GROUP, cols]
            place = lax.broadcasted_iota(jnp.int32, (GROUP, DV), 0)
            recalled = jnp.zeros((GROUP, DV), f32)
            for j in range(GROUP):
                stored = memory_ref[r + j, h].astype(bf)
                one = lax.dot_general(some, stored, transposed, preferred_element_type=f32)
                recalled = jnp.where(place == j, one, recalled)
            groups.append(recalled)
        recalled = jnp.concatenate(groups, axis=0)
        numer = keep * recalled + (admit * match) * values[:, vcols].astype(f32)
        cell = numer / jnp.maximum(jnp.abs(denom), 1.0)
        gate = jax.nn.sigmoid(gate_out[:, vcols].astype(f32))
        mixed_ref[:, vcols] = (cell * memory_gain_ref[:, vcols] * gate).astype(bf)
    keep_ref[...] = keep_all
    admit_ref[...] = admit_all


def fetch_kernel(count, *refs):
    copies = [
        pltpu.make_async_copy(refs[i], refs[count + i], refs[2 * count].at[i]) for i in range(count)
    ]
    for copy in copies:
        copy.start()
    for copy in copies:
        copy.wait()


def fetch(*args):
    args = [pltpu.with_memory_space_constraint(a, pltpu.HBM) for a in args]
    return pl.pallas_call(
        functools.partial(fetch_kernel, len(args)),
        out_shape=[pltpu.VMEM(a.shape, a.dtype) for a in args],
        in_specs=[pl.BlockSpec(memory_space=pltpu.HBM)] * len(args),
        out_specs=[pl.BlockSpec(memory_space=pltpu.VMEM)] * len(args),
        scratch_shapes=[pltpu.SemaphoreType.DMA((len(args),))],
        compiler_params=pltpu.CompilerParams(vmem_limit_bytes=2**20),
        cost_estimate=pl.CostEstimate(flops=10**9, bytes_accessed=9 * 2**20, transcendentals=0),
        name="fetch",
    )(*args)


def run_cell(blocks, heads, *args):
    own, f32 = blocks[0].shape[0], jnp.float32
    args = [pltpu.with_memory_space_constraint(a, pltpu.VMEM) for a in args]
    shapes = [
        ((own, heads * DV), jnp.bfloat16),
        ((own, heads, DK), f32),
        ((heads, own), f32),
        ((own, heads), f32),
        ((own, heads), f32),
        ((own, heads * DK), jnp.bfloat16),
        ((own, heads * DV), jnp.bfloat16),
    ]
    in_vmem = pl.BlockSpec(memory_space=pltpu.VMEM)
    return pl.pallas_call(
        functools.partial(cell_kernel, heads),
        out_shape=[jax.ShapeDtypeStruct(*s) for s in shapes],
        in_specs=[in_vmem] * (len(blocks) + len(args)),
        out_specs=[in_vmem] * len(shapes),
        compiler_params=pltpu.CompilerParams(vmem_limit_bytes=8 * 2**20),
        cost_estimate=pl.CostEstimate(flops=10**9, bytes_accessed=9 * 2**20, transcendentals=0),
        name="cell",
    )(*blocks, *args)


STEP = 4


def update_kernel(
    memory_ref,
    keep_ref,
    admit_ref,
    keys_ref,
    values_ref,
    proj_ref,
    out_ref,
    held_ref,
    staged_ref,
    sems,
    held_sem,
):
    f32 = jnp.float32
    rows, heads = memory_ref.shape[:2]
    held = pltpu.make_async_copy(proj_ref, held_ref, held_sem)
    held.start()
    values = values_ref[...].astype(f32)
    values = jnp.concatenate([values, jnp.zeros((128 - rows, values.shape[1]), f32)], axis=0)
    columns = [jnp.transpose(values[:, h * DV : (h + 1) * DV]) for h in range(heads)]
    keys = keys_ref[...].astype(f32) * DK ** (-0.5)
    copies = []
    for r in range(rows):
        for h in range(heads):
            key = keys[r : r + 1, h * DK : (h + 1) * DK] * admit_ref[r : r + 1, h : h + 1]
            added = columns[h][:, r : r + 1] * key
            staged_ref[r, h] = keep_ref[r : r + 1, h : h + 1] * memory_ref[r, h] + added
        if r % STEP == STEP - 1:
            part = pl.ds(r - STEP + 1, STEP)
            copy = pltpu.make_async_copy(staged_ref.at[part], out_ref.at[part], sems.at[r // STEP])
            copy.start()
            copies.append(copy)
    for copy in copies:
        copy.wait()
    held.wait()


def run_update(memory, keep, admit, keys, values, proj):
    in_vmem = pl.BlockSpec(memory_space=pltpu.VMEM)
    args = [pltpu.with_memory_space_constraint(a, pltpu.VMEM) for a in (memory, keep, admit, keys, values)]
    args.append(pltpu.with_memory_space_constraint(proj, pltpu.HBM))
    return pl.pallas_call(
        update_kernel,
        out_shape=[
            pltpu.HBM(memory.shape, memory.dtype),
            pltpu.VMEM(proj.shape, proj.dtype),
        ],
        in_specs=[in_vmem] * 5 + [pl.BlockSpec(memory_space=pltpu.HBM)],
        out_specs=[pl.BlockSpec(memory_space=pltpu.HBM), in_vmem],
        scratch_shapes=[
            pltpu.VMEM(memory.shape, memory.dtype),
            pltpu.SemaphoreType.DMA((memory.shape[0] // STEP,)),
            pltpu.SemaphoreType.DMA,
        ],
        compiler_params=pltpu.CompilerParams(vmem_limit_bytes=12 * 2**20),
        cost_estimate=pl.CostEstimate(flops=10**9, bytes_accessed=9 * 2**20, transcendentals=0),
        name="update",
    )(*args)


def second_kernel(*refs):
    blocks = lax.axis_size("tp")
    proj_ref, tokens_ref, sent_ref, second_ref, square_ref = refs[blocks:]
    f32 = jnp.float32
    width = refs[0].shape[1]
    me = lax.axis_index("tp")
    total = tokens_ref[...].astype(f32)
    for b in range(blocks):
        at = pl.ds(pl.multiple_of((me ^ b) * width, width), width)
        total += jnp.dot(refs[b][...], proj_ref[at, :], preferred_element_type=f32)
    second = total.astype(jnp.bfloat16)
    second_ref[...] = second
    for i in range(sent_ref.shape[0]):
        sent_ref[i] = second
    second = second.astype(f32)
    square_ref[...] = jnp.sum(second * second, axis=1, keepdims=True)


def run_second(blocks, proj, tokens, copies):
    in_vmem = pl.BlockSpec(memory_space=pltpu.VMEM)
    args = [pltpu.with_memory_space_constraint(a, pltpu.VMEM) for a in (*blocks, proj, tokens)]
    return pl.pallas_call(
        second_kernel,
        out_shape=[
            jax.ShapeDtypeStruct((copies,) + tokens.shape, jnp.bfloat16),
            jax.ShapeDtypeStruct(tokens.shape, jnp.bfloat16),
            jax.ShapeDtypeStruct((tokens.shape[0], 1), jnp.float32),
        ],
        in_specs=[in_vmem] * len(args),
        out_specs=[in_vmem] * 3,
        compiler_params=pltpu.CompilerParams(vmem_limit_bytes=4 * 2**20),
        cost_estimate=pl.CostEstimate(flops=10**8, bytes_accessed=2**21, transcendentals=0),
        name="second",
    )(*args)


def up_kernel(rows_ref, gain_ref, up_ref, *out_refs):
    f32 = jnp.float32
    side = lax.axis_index("tp") & 1
    half = up_ref.shape[1] // 2
    own, theirs = (pl.ds(pl.multiple_of(s * half, half), half) for s in (side, 1 - side))
    groups = rows_ref.shape[0] // CHUNKS
    for c in range(CHUNKS):
        rows = rows_ref[c * groups : (c + 1) * groups].astype(f32) * gain_ref[...]
        rows = rows.reshape(-1, rows.shape[-1]).astype(jnp.bfloat16)
        away = jnp.dot(rows, up_ref[:, theirs], preferred_element_type=f32)
        out_refs[c][...] = away.astype(jnp.bfloat16)
        out_refs[CHUNKS + c][...] = jnp.dot(rows, up_ref[:, own], preferred_element_type=f32)


def run_up(rows, gain, up):
    in_vmem = pl.BlockSpec(memory_space=pltpu.VMEM)
    shape = (rows.shape[0] * rows.shape[1] // CHUNKS, up.shape[1] // 2)
    outs = pl.pallas_call(
        up_kernel,
        out_shape=[jax.ShapeDtypeStruct(shape, jnp.bfloat16)] * CHUNKS
        + [jax.ShapeDtypeStruct(shape, jnp.float32)] * CHUNKS,
        in_specs=[in_vmem] * 3,
        out_specs=[in_vmem] * (2 * CHUNKS),
        compiler_params=pltpu.CompilerParams(vmem_limit_bytes=8 * 2**20),
        cost_estimate=pl.CostEstimate(flops=10**9, bytes_accessed=2**21, transcendentals=0),
        name="up",
    )(rows, gain, up)
    return outs[:CHUNKS], outs[CHUNKS:]


def halves(down_ref):
    side = lax.axis_index("tp") & 1
    half = down_ref.shape[0] // 2
    return (down_ref[pl.ds(pl.multiple_of(s * half, half), half), :] for s in (side, 1 - side))


def down_kernel(*refs):
    f32 = jnp.float32
    *inputs, down_ref, out_ref = refs
    hidden, other = inputs[:CHUNKS], inputs[CHUNKS:]
    own, theirs = halves(down_ref)
    step = hidden[0].shape[0]
    for c in range(CHUNKS):
        total = jnp.dot(hidden[c][...], own, preferred_element_type=f32)
        if c < len(other):
            total += jnp.dot(other[c][...], theirs, preferred_element_type=f32)
        out_ref[c * step : (c + 1) * step, :] = total


def last_kernel(partial_ref, other_ref, down_ref, out_ref):
    _, theirs = halves(down_ref)
    begin = partial_ref.shape[0] - other_ref.shape[0]
    last = partial_ref[begin:, :]
    last += jnp.dot(other_ref[...], theirs, preferred_element_type=jnp.float32)
    own = out_ref.shape[1]
    groups = begin // own
    out_ref[:groups] = partial_ref[:begin, :].reshape(groups, own, -1).astype(jnp.bfloat16)
    out_ref[groups:] = last.reshape(out_ref.shape[0] - groups, own, -1).astype(jnp.bfloat16)


def run_down(kernel, name, shape, dtype, *args):
    in_vmem = pl.BlockSpec(memory_space=pltpu.VMEM)
    return pl.pallas_call(
        kernel,
        out_shape=jax.ShapeDtypeStruct(shape, dtype),
        in_specs=[in_vmem] * len(args),
        out_specs=in_vmem,
        compiler_params=pltpu.CompilerParams(vmem_limit_bytes=8 * 2**20),
        cost_estimate=pl.CostEstimate(flops=10**8, bytes_accessed=2**21, transcendentals=0),
        name=name,
    )(*args)


def swap(array, bit):
    pairs = [(i, i ^ bit) for i in range(lax.axis_size("tp"))]
    return lax.ppermute(array, "tp", pairs)


def per_device(
    tokens,
    memory,
    normalizer,
    stabilizer,
    norm_gain,
    query_weight,
    key_weight,
    value_weight,
    outgate_weight,
    input_gate_weight,
    forget_gate_weight,
    forget_bias,
    memory_gain,
    proj_weight,
    ffn_gain,
    up_weight,
    down_weight,
):
    own_rows = tokens.shape[0]
    heads_here = memory.shape[1]
    blocks = [tokens] + [swap(tokens, b) for b in reversed(range(1, lax.axis_size("tp")))][::-1]
    held = fetch(
        norm_gain.reshape(1, -1),
        query_weight,
        key_weight,
        value_weight,
        outgate_weight,
        input_gate_weight.T,
        forget_gate_weight.T,
        forget_bias.reshape(1, -1),
        stabilizer.T,
        normalizer,
        memory,
        memory_gain.reshape(1, -1),
    )
    mixed, normalizer_new, stab_new, keep, admit, keys, values = run_cell(blocks, heads_here, *held)
    stab_new = stab_new.T
    kv, tp = lax.axis_size("kv"), lax.axis_size("tp")
    mixed_blocks = [mixed] + [swap(mixed, b) for b in range(1, tp)]
    memory_new, proj_held = run_update(held[10], keep, admit, keys, values, proj_weight)
    sent, second, square_sum = run_second(mixed_blocks, proj_held, tokens, kv)
    all_rows = lax.all_to_all(sent, "kv", 0, 0, tiled=True)
    away, kept = run_up(all_rows, ffn_gain.reshape(1, -1), up_weight)
    came = [swap(a, 1) for a in away]
    came[0], square_sum = lax.optimization_barrier((came[0], square_sum))
    sent = [(k + c.astype(jnp.float32)).astype(jnp.bfloat16) for k, c in zip(kept, came)]
    square_sum = square_sum + swap(square_sum, 1)
    sent[-1], square_sum = lax.optimization_barrier((sent[-1], square_sum))
    bit = 2
    while bit < tp:
        came = [swap(x, bit) for x in sent]
        square_sum = square_sum + swap(square_sum, bit)
        came[-1], square_sum = lax.optimization_barrier((came[-1], square_sum))
        preact = [x.astype(jnp.float32) + y.astype(jnp.float32) for x, y in zip(sent, came)]
        sent = [p.astype(jnp.bfloat16) for p in preact]
        bit *= 2
    hidden = [jnp.square(jax.nn.relu(p)).astype(jnp.bfloat16) for p in preact]
    other = [swap(h, 1) for h in hidden]
    shape = (kv * own_rows, second.shape[1])
    partial = run_down(
        down_kernel, "down", shape, jnp.float32, *hidden, *other[:-1], down_weight
    )
    sent = run_down(
        last_kernel, "last", (kv, own_rows, shape[1]), jnp.bfloat16, partial, other[-1], down_weight
    )
    scale_two = lax.rsqrt(square_sum / D + EPS)
    factor = jnp.broadcast_to(scale_two * scale_two, second.shape)
    sent, factor, second = lax.optimization_barrier((sent, factor, second))
    got = lax.all_to_all(sent, "kv", 0, 0, tiled=True)
    summed = jnp.sum(got.astype(jnp.float32), axis=0)
    layer_out = (second.astype(jnp.float32) + summed * factor).astype(jnp.bfloat16)
    return (layer_out, memory_new, normalizer_new, stab_new)


def solution(mesh):
    placed = (
        P("kv", "tp"),
        P("kv", "tp", None, None),
        P("kv", "tp", None),
        P("kv", "tp"),
        P(),
        P(None, "tp"),
        P(None, "tp"),
        P(None, "tp"),
        P(None, "tp"),
        P(),
        P(),
        P(),
        P("tp"),
        P(None, "tp"),
        P("tp"),
        P("tp", "kv"),
        P("kv", "tp"),
    )
    return jax.shard_map(
        per_device,
        mesh=mesh,
        in_specs=placed,
        out_specs=(P("kv", "tp"), P("kv", "tp", None, None), P("kv", "tp", None), P("kv", "tp")),
        check_vma=False,
    )
```

```python
import functools
import jax
import jax.numpy as jnp
from jax import lax
from jax.experimental import pallas as pl
from jax.experimental.pallas import tpu as pltpu
from jax.sharding import PartitionSpec as P

D = 2048
DK = 128
DV = 128


EPS = 1e-06


GROUP = 16


def cell_kernel(
    heads,
    *refs,
):
    blocks = lax.axis_size("tp")
    cell_body(heads, refs[:blocks], *refs[blocks:])


def cell_body(
    heads,
    rows_refs,
    gain_ref,
    query_ref,
    key_ref,
    value_ref,
    outgate_ref,
    input_ref,
    forget_ref,
    bias_ref,
    stabilizer_ref,
    normalizer_ref,
    memory_ref,
    memory_gain_ref,
    mixed_ref,
    normalizer_new_ref,
    stab_new_ref,
    keep_ref,
    admit_ref,
    keys_out_ref,
    values_out_ref,
):
    bf, f32 = jnp.bfloat16, jnp.float32
    first_head = lax.axis_index("tp") * heads
    me = lax.axis_index("tp")
    width = rows_refs[0].shape[1]
    squares = [jnp.square(ref[...].astype(f32)) for ref in rows_refs]
    squares = [jnp.sum(s, axis=-1, keepdims=True) for s in squares]
    scale_one = lax.rsqrt(sum(squares) / (width * len(squares)) + EPS)
    transposed = (((1,), (1,)), ((), ()))
    sums = [0.0] * 6
    for b, ref in enumerate(rows_refs):
        at = pl.ds(pl.multiple_of((me ^ b) * width, width), width)
        normed = (ref[...].astype(f32) * scale_one * gain_ref[:, at]).astype(bf)
        for n, w in enumerate((input_ref, forget_ref)):
            sums[n] += lax.dot_general(normed, w[:, at], transposed, preferred_element_type=f32)
        for n, w in enumerate((key_ref, query_ref, value_ref, outgate_ref)):
            sums[2 + n] += jnp.dot(normed, w[at, :], preferred_element_type=f32)
    input_all = sums[0]
    forget_all = jax.nn.log_sigmoid(sums[1] + bias_ref[...])
    keys, query, values, gate_out = (s.astype(bf) for s in sums[2:])
    keys_out_ref[...] = keys
    values_out_ref[...] = values
    lane = lax.broadcasted_iota(jnp.int32, input_all.shape, 1)
    count = rows_refs[0].shape[0]
    own = lax.broadcasted_iota(jnp.int32, keep_ref.shape, 1)
    diagonal = lax.broadcasted_iota(jnp.int32, (count, count), 0) == lax.broadcasted_iota(
        jnp.int32, (count, count), 1
    )
    keep_all, admit_all = (jnp.zeros(keep_ref.shape, f32) for _ in range(2))
    for h in range(heads):
        chosen = lane == first_head + h
        input_log = jnp.sum(jnp.where(chosen, input_all, 0.0), axis=1, keepdims=True)
        forget_log = jnp.sum(jnp.where(chosen, forget_all, 0.0), axis=1, keepdims=True)
        before = jnp.where(diagonal, stabilizer_ref[h : h + 1, :], 0.0)
        decayed = forget_log + jnp.sum(before, axis=1, keepdims=True)
        stab = jnp.maximum(decayed, input_log)
        keep = jnp.exp(decayed - stab)
        admit = jnp.exp(input_log - stab)
        stab_new_ref[h : h + 1, :] = jnp.sum(jnp.where(diagonal, stab, 0.0), axis=0, keepdims=True)
        keep_all = jnp.where(own == h, keep, keep_all)
        admit_all = jnp.where(own == h, admit, admit_all)
        cols = slice(h * DK, (h + 1) * DK)
        vcols = slice(h * DV, (h + 1) * DV)
        keys_f = keys[:, cols].astype(f32) * DK ** (-0.5)
        query_f = query[:, cols].astype(f32)
        normalizer_new = keep * normalizer_ref[:, h, :] + admit * keys_f
        normalizer_new_ref[:, h, :] = normalizer_new
        denom = jnp.sum(normalizer_new * query_f, axis=-1, keepdims=True)
        match = jnp.sum(keys_f * query_f, axis=-1, keepdims=True)
        groups = []
        for r in range(0, count, GROUP):
            some = query[r : r + GROUP, cols]
            place = lax.broadcasted_iota(jnp.int32, (GROUP, DV), 0)
            recalled = jnp.zeros((GROUP, DV), f32)
            for j in range(GROUP):
                stored = memory_ref[r + j, h].astype(bf)
                one = lax.dot_general(some, stored, transposed, preferred_element_type=f32)
                recalled = jnp.where(place == j, one, recalled)
            groups.append(recalled)
        recalled = jnp.concatenate(groups, axis=0)
        numer = keep * recalled + (admit * match) * values[:, vcols].astype(f32)
        cell = numer / jnp.maximum(jnp.abs(denom), 1.0)
        gate = jax.nn.sigmoid(gate_out[:, vcols].astype(f32))
        mixed_ref[:, vcols] = (cell * memory_gain_ref[:, vcols] * gate).astype(bf)
    keep_ref[...] = keep_all
    admit_ref[...] = admit_all


def fetch_kernel(count, *refs):
    copies = [
        pltpu.make_async_copy(refs[i], refs[count + i], refs[2 * count].at[i]) for i in range(count)
    ]
    for copy in copies:
        copy.start()
    for copy in copies:
        copy.wait()


def fetch(*args):
    args = [pltpu.with_memory_space_constraint(a, pltpu.HBM) for a in args]
    return pl.pallas_call(
        functools.partial(fetch_kernel, len(args)),
        out_shape=[pltpu.VMEM(a.shape, a.dtype) for a in args],
        in_specs=[pl.BlockSpec(memory_space=pltpu.HBM)] * len(args),
        out_specs=[pl.BlockSpec(memory_space=pltpu.VMEM)] * len(args),
        scratch_shapes=[pltpu.SemaphoreType.DMA((len(args),))],
        compiler_params=pltpu.CompilerParams(vmem_limit_bytes=2**20),
        cost_estimate=pl.CostEstimate(flops=10**9, bytes_accessed=9 * 2**20, transcendentals=0),
        name="fetch",
    )(*args)


def run_cell(blocks, heads, *args):
    own, f32 = blocks[0].shape[0], jnp.float32
    args = [pltpu.with_memory_space_constraint(a, pltpu.VMEM) for a in args]
    shapes = [
        ((own, heads * DV), jnp.bfloat16),
        ((own, heads, DK), f32),
        ((heads, own), f32),
        ((own, heads), f32),
        ((own, heads), f32),
        ((own, heads * DK), jnp.bfloat16),
        ((own, heads * DV), jnp.bfloat16),
    ]
    in_vmem = pl.BlockSpec(memory_space=pltpu.VMEM)
    return pl.pallas_call(
        functools.partial(cell_kernel, heads),
        out_shape=[jax.ShapeDtypeStruct(*s) for s in shapes],
        in_specs=[in_vmem] * (len(blocks) + len(args)),
        out_specs=[in_vmem] * len(shapes),
        compiler_params=pltpu.CompilerParams(vmem_limit_bytes=8 * 2**20),
        cost_estimate=pl.CostEstimate(flops=10**9, bytes_accessed=9 * 2**20, transcendentals=0),
        name="cell",
    )(*blocks, *args)


STEP = 4
EARLY = 4


def update_rows(rows, memory_ref, keep_ref, admit_ref, keys_ref, values_ref, staged_ref, emit):
    f32 = jnp.float32
    count, heads = keep_ref.shape
    values = values_ref[...].astype(f32)
    values = jnp.concatenate([values, jnp.zeros((128 - count, values.shape[1]), f32)], axis=0)
    columns = [jnp.transpose(values[:, h * DV : (h + 1) * DV]) for h in range(heads)]
    keys = keys_ref[...].astype(f32) * DK ** (-0.5)
    for n, r in enumerate(rows):
        if emit is not None and n % STEP == 0:
            emit("need", n)
        for h in range(heads):
            key = keys[r : r + 1, h * DK : (h + 1) * DK] * admit_ref[r : r + 1, h : h + 1]
            added = columns[h][:, r : r + 1] * key
            staged_ref[n, h] = keep_ref[r : r + 1, h : h + 1] * memory_ref[n, h] + added
        if n % STEP == STEP - 1:
            emit("done", n)


def update_kernel(rows, early, count, *refs):
    if early:
        memory_ref, *small = refs[:5]
        given, refs = refs[5 : 5 + count], refs[5 + count :]
        out_ref, held_refs, refs = refs[0], refs[1 : 1 + count], refs[1 + count :]
        staged_ref, sems, held_sems = refs
    else:
        memory_hbm, *small = refs[1:6]
        given, refs = refs[6 : 6 + count], refs[6 + count :]
        out_ref, held_refs, refs = refs[0], refs[1 : 1 + count], refs[1 + count :]
        staged_ref, sems, held_sems, memory_ref, in_sems = refs
    parts = [pl.ds(n, STEP) for n in range(0, len(rows), STEP)]
    places = [pl.ds(rows[n], STEP) for n in range(0, len(rows), STEP)]
    outward = [
        pltpu.make_async_copy(staged_ref.at[p], out_ref.at[q], sems.at[n])
        for n, (p, q) in enumerate(zip(parts, places))
    ]
    inward = []
    if not early:
        inward = [
            pltpu.make_async_copy(memory_hbm.at[q], memory_ref.at[p], in_sems.at[n])
            for n, (p, q) in enumerate(zip(parts, places))
        ]
    held = [
        pltpu.make_async_copy(a, b, held_sems.at[n])
        for n, (a, b) in enumerate(zip(given, held_refs))
    ]
    for copy in inward + held:
        copy.start()

    def emit(what, n):
        if what == "need" and inward:
            inward[n // STEP].wait()
        if what == "done":
            outward[n // STEP].start()

    update_rows(rows, memory_ref, *small, staged_ref, emit)
    for copy in outward + held:
        copy.wait()


def run_update(memory, small, weights, before=None, rows=()):
    vmem, hbm = pl.BlockSpec(memory_space=pltpu.VMEM), pl.BlockSpec(memory_space=pltpu.HBM)
    early = before is None
    staged = pltpu.VMEM((len(rows),) + memory.shape[1:], memory.dtype)
    sems = pltpu.SemaphoreType.DMA((len(rows) // STEP,))
    scratch = [staged, sems, pltpu.SemaphoreType.DMA((len(weights),))]
    if early:
        args = [pltpu.with_memory_space_constraint(a, pltpu.VMEM) for a in (memory, *small)]
        in_specs = [vmem] * len(args)
    else:
        args = [pltpu.with_memory_space_constraint(a, pltpu.HBM) for a in (before, memory)]
        args += list(small)
        in_specs = [hbm] * 2 + [vmem] * len(small)
        scratch += [staged, sems]
    args += [pltpu.with_memory_space_constraint(w, pltpu.HBM) for w in weights]
    return pl.pallas_call(
        functools.partial(update_kernel, rows, early, len(weights)),
        out_shape=[pltpu.HBM(memory.shape, memory.dtype)]
        + [pltpu.VMEM(w.shape, w.dtype) for w in weights],
        in_specs=in_specs + [hbm] * len(weights),
        out_specs=[hbm] + [vmem] * len(weights),
        scratch_shapes=scratch,
        input_output_aliases={} if early else {0: 0},
        compiler_params=pltpu.CompilerParams(vmem_limit_bytes=12 * 2**20),
        cost_estimate=pl.CostEstimate(flops=10**9, bytes_accessed=9 * 2**20, transcendentals=0),
        name="update" if early else "update_rest",
    )(*args)


def second_kernel(*refs):
    blocks = lax.axis_size("tp")
    projs, tokens = refs[blocks : blocks + 2], refs[blocks + 2 : blocks + 4]
    sent_ref, second_ref, square_ref = refs[blocks + 4 :]
    f32 = jnp.float32
    me = lax.axis_index("tp")
    part = second_ref.shape[0]
    rows = pl.ds(pl.multiple_of((me & 1) * part, part), part)
    width, columns = refs[0].shape[1], tokens[0].shape[1]
    square = 0.0
    for n in range(2):
        total = tokens[n][rows, :].astype(f32)
        for b in range(blocks):
            at = pl.ds(pl.multiple_of((me ^ b) * width, width), width)
            total += jnp.dot(refs[b][rows, :], projs[n][at, :], preferred_element_type=f32)
        second = total.astype(jnp.bfloat16)
        cols = slice(n * columns, (n + 1) * columns)
        second_ref[:, cols] = second
        for i in range(sent_ref.shape[0]):
            sent_ref[i, :, cols] = second
        second = second.astype(f32)
        square += jnp.sum(second * second, axis=1, keepdims=True)
    square_ref[...] = square


def up_kernel(rows_ref, gain_ref, gain_other_ref, up_ref, up_other_ref, out_ref):
    f32 = jnp.float32
    total = 0.0
    width = up_ref.shape[0]
    for n, (gain, up) in enumerate(((gain_ref, up_ref), (gain_other_ref, up_other_ref))):
        rows = rows_ref[:, :, n * width : (n + 1) * width].astype(f32) * gain[...]
        rows = rows.reshape(-1, width).astype(jnp.bfloat16)
        total += jnp.dot(rows, up[...], preferred_element_type=f32)
    out_ref[...] = total.astype(jnp.bfloat16)


def down_kernel(sent_ref, came_ref, down_ref, down_other_ref, out_ref):
    f32 = jnp.float32
    preact = sent_ref[...].astype(f32) + came_ref[...].astype(f32)
    hidden = jnp.square(jnp.maximum(preact, 0.0)).astype(jnp.bfloat16)
    width = down_ref.shape[1]
    for n, down in enumerate((down_ref, down_other_ref)):
        partial = jnp.dot(hidden, down[...], preferred_element_type=f32).astype(jnp.bfloat16)
        partial = partial.reshape(out_ref.shape[0], out_ref.shape[1], width)
        out_ref[:, :, n * width : (n + 1) * width] = partial


def run_plain(kernel, name, shapes, held, *args):
    in_vmem = pl.BlockSpec(memory_space=pltpu.VMEM)
    args = [
        pltpu.with_memory_space_constraint(a, pltpu.VMEM) if n < held else a
        for n, a in enumerate(args)
    ]
    return pl.pallas_call(
        kernel,
        out_shape=[jax.ShapeDtypeStruct(*s) for s in shapes],
        in_specs=[in_vmem] * len(args),
        out_specs=[in_vmem] * len(shapes),
        compiler_params=pltpu.CompilerParams(vmem_limit_bytes=8 * 2**20),
        cost_estimate=pl.CostEstimate(flops=10**9, bytes_accessed=2**21, transcendentals=0),
        name=name,
    )(*args)


def swap(array, bit):
    pairs = [(i, i ^ bit) for i in range(lax.axis_size("tp"))]
    return lax.ppermute(array, "tp", pairs)


def per_device(
    tokens,
    memory,
    normalizer,
    stabilizer,
    norm_gain,
    query_weight,
    key_weight,
    value_weight,
    outgate_weight,
    input_gate_weight,
    forget_gate_weight,
    forget_bias,
    memory_gain,
    proj_weight,
    ffn_gain,
    up_weight,
    down_weight,
):
    own_rows = tokens.shape[0]
    heads_here = memory.shape[1]
    blocks = [tokens] + [swap(tokens, b) for b in reversed(range(1, lax.axis_size("tp")))][::-1]
    proj_other, gain_other, up_other = (
        swap(w, 1) for w in (proj_weight, ffn_gain.reshape(1, -1), up_weight)
    )
    held = fetch(
        norm_gain.reshape(1, -1),
        query_weight,
        key_weight,
        value_weight,
        outgate_weight,
        input_gate_weight.T,
        forget_gate_weight.T,
        forget_bias.reshape(1, -1),
        stabilizer.T,
        normalizer,
        memory,
        memory_gain.reshape(1, -1),
    )
    mixed, normalizer_new, stab_new, keep, admit, keys, values = run_cell(blocks, heads_here, *held)
    stab_new = stab_new.T
    kv, tp = lax.axis_size("kv"), lax.axis_size("tp")
    bf, f32 = jnp.bfloat16, jnp.float32
    up_other = pltpu.with_memory_space_constraint(up_other, pltpu.VMEM)
    mixed, gain_other, up_other = lax.optimization_barrier((mixed, gain_other, up_other))
    mixed_blocks = [mixed] + [swap(mixed, b) for b in range(1, tp)]
    small = (keep, admit, keys, values)
    begun = tuple(range(own_rows * EARLY // 8))
    memory_part, proj_held = run_update(held[10], small, (proj_weight,), rows=begun)
    part, columns = own_rows // 2, 2 * tokens.shape[1]
    shapes = [((kv, part, columns), bf), ((part, columns), bf), ((part, 1), f32)]
    sent, second, square_sum = run_plain(
        second_kernel, "second", shapes, tp + 4, *mixed_blocks, proj_held, proj_other, *blocks[:2]
    )
    rows = lax.all_to_all(sent, "kv", 0, 0, tiled=True)
    gains = (ffn_gain.reshape(1, -1), gain_other)
    shapes = [((kv * part, up_weight.shape[1]), bf)]
    (sent,) = run_plain(up_kernel, "up", shapes, 0, rows, *gains, up_weight, up_other)
    sent, small, square_sum, down_weight = lax.optimization_barrier(
        (sent, small, square_sum, down_weight)
    )
    down_other = swap(down_weight, 1)
    memory_new, down_held = run_update(
        memory,
        small,
        (down_weight,),
        before=memory_part,
        rows=tuple(range(len(begun), own_rows)),
    )
    bit = 2
    while bit < tp:
        if bit > 2:
            sent = (sent.astype(f32) + came.astype(f32)).astype(bf)
        came = swap(sent, bit)
        square_sum = square_sum + swap(square_sum, bit)
        bit *= 2
    scale_two = lax.rsqrt(square_sum / D + EPS)
    factor = jnp.broadcast_to(scale_two * scale_two, second.shape)
    came, memory_new, factor, second = lax.optimization_barrier((came, memory_new, factor, second))
    shapes = [((kv, part, columns), bf)]
    (sent,) = run_plain(
        down_kernel, "down", shapes, 0, sent, came, down_held, down_other
    )
    got = lax.all_to_all(sent, "kv", 0, 0, tiled=True)
    summed = jnp.sum(got.astype(f32), axis=0)
    done = (second.astype(f32) + summed * factor).astype(bf)
    kept, given = jnp.split(done, 2, axis=1)
    taken = swap(given, 1)
    first = (lax.axis_index("tp") & 1) == 0
    layer_out = jnp.concatenate(
        [jnp.where(first, kept, taken), jnp.where(first, taken, kept)], axis=0
    )
    return (layer_out, memory_new, normalizer_new, stab_new)


def solution(mesh):
    placed = (
        P("kv", "tp"),
        P("kv", "tp", None, None),
        P("kv", "tp", None),
        P("kv", "tp"),
        P(),
        P(None, "tp"),
        P(None, "tp"),
        P(None, "tp"),
        P(None, "tp"),
        P(),
        P(),
        P(),
        P("tp"),
        P(None, "tp"),
        P("tp"),
        P("tp", "kv"),
        P("kv", "tp"),
    )
    return jax.shard_map(
        per_device,
        mesh=mesh,
        in_specs=placed,
        out_specs=(P("kv", "tp"), P("kv", "tp", None, None), P("kv", "tp", None), P("kv", "tp")),
        check_vma=False,
    )
```

```python
import functools
import jax
import jax.numpy as jnp
from jax import lax
from jax.experimental import pallas as pl
from jax.experimental.pallas import tpu as pltpu
from jax.sharding import PartitionSpec as P

D = 2048
DK = 128
DV = 128


EPS = 1e-06


GROUP = 16


def cell_kernel(
    heads,
    *refs,
):
    blocks = lax.axis_size("tp")
    cell_body(heads, refs[:blocks], *refs[blocks:])


def cell_body(
    heads,
    rows_refs,
    gain_ref,
    query_ref,
    key_ref,
    value_ref,
    outgate_ref,
    input_ref,
    forget_ref,
    bias_ref,
    stabilizer_ref,
    normalizer_ref,
    memory_ref,
    memory_gain_ref,
    mixed_ref,
    normalizer_new_ref,
    stab_new_ref,
    keep_ref,
    admit_ref,
    keys_out_ref,
    values_out_ref,
):
    bf, f32 = jnp.bfloat16, jnp.float32
    first_head = lax.axis_index("tp") * heads
    me = lax.axis_index("tp")
    width = rows_refs[0].shape[1]
    squares = [jnp.square(ref[...].astype(f32)) for ref in rows_refs]
    squares = [jnp.sum(s, axis=-1, keepdims=True) for s in squares]
    scale_one = lax.rsqrt(sum(squares) / (width * len(squares)) + EPS)
    transposed = (((1,), (1,)), ((), ()))
    sums = [0.0] * 6
    for b, ref in enumerate(rows_refs):
        at = pl.ds(pl.multiple_of((me ^ b) * width, width), width)
        normed = (ref[...].astype(f32) * scale_one * gain_ref[:, at]).astype(bf)
        for n, w in enumerate((input_ref, forget_ref)):
            sums[n] += lax.dot_general(normed, w[:, at], transposed, preferred_element_type=f32)
        for n, w in enumerate((key_ref, query_ref, value_ref, outgate_ref)):
            sums[2 + n] += jnp.dot(normed, w[at, :], preferred_element_type=f32)
    input_all = sums[0]
    forget_all = jax.nn.log_sigmoid(sums[1] + bias_ref[...])
    keys, query, values, gate_out = (s.astype(bf) for s in sums[2:])
    keys_out_ref[...] = keys
    values_out_ref[...] = values
    lane = lax.broadcasted_iota(jnp.int32, input_all.shape, 1)
    count = rows_refs[0].shape[0]
    own = lax.broadcasted_iota(jnp.int32, keep_ref.shape, 1)
    diagonal = lax.broadcasted_iota(jnp.int32, (count, count), 0) == lax.broadcasted_iota(
        jnp.int32, (count, count), 1
    )
    keep_all, admit_all = (jnp.zeros(keep_ref.shape, f32) for _ in range(2))
    for h in range(heads):
        chosen = lane == first_head + h
        input_log = jnp.sum(jnp.where(chosen, input_all, 0.0), axis=1, keepdims=True)
        forget_log = jnp.sum(jnp.where(chosen, forget_all, 0.0), axis=1, keepdims=True)
        before = jnp.where(diagonal, stabilizer_ref[h : h + 1, :], 0.0)
        decayed = forget_log + jnp.sum(before, axis=1, keepdims=True)
        stab = jnp.maximum(decayed, input_log)
        keep = jnp.exp(decayed - stab)
        admit = jnp.exp(input_log - stab)
        stab_new_ref[h : h + 1, :] = jnp.sum(jnp.where(diagonal, stab, 0.0), axis=0, keepdims=True)
        keep_all = jnp.where(own == h, keep, keep_all)
        admit_all = jnp.where(own == h, admit, admit_all)
        cols = slice(h * DK, (h + 1) * DK)
        vcols = slice(h * DV, (h + 1) * DV)
        keys_f = keys[:, cols].astype(f32) * DK ** (-0.5)
        query_f = query[:, cols].astype(f32)
        normalizer_new = keep * normalizer_ref[:, h, :] + admit * keys_f
        normalizer_new_ref[:, h, :] = normalizer_new
        denom = jnp.sum(normalizer_new * query_f, axis=-1, keepdims=True)
        match = jnp.sum(keys_f * query_f, axis=-1, keepdims=True)
        groups = []
        for r in range(0, count, GROUP):
            some = query[r : r + GROUP, cols]
            place = lax.broadcasted_iota(jnp.int32, (GROUP, DV), 0)
            recalled = jnp.zeros((GROUP, DV), f32)
            for j in range(GROUP):
                stored = memory_ref[r + j, h].astype(bf)
                one = lax.dot_general(some, stored, transposed, preferred_element_type=f32)
                recalled = jnp.where(place == j, one, recalled)
            groups.append(recalled)
        recalled = jnp.concatenate(groups, axis=0)
        numer = keep * recalled + (admit * match) * values[:, vcols].astype(f32)
        cell = numer / jnp.maximum(jnp.abs(denom), 1.0)
        gate = jax.nn.sigmoid(gate_out[:, vcols].astype(f32))
        mixed_ref[:, vcols] = (cell * memory_gain_ref[:, vcols] * gate).astype(bf)
    keep_ref[...] = keep_all
    admit_ref[...] = admit_all


def fetch_kernel(count, *refs):
    copies = [
        pltpu.make_async_copy(refs[i], refs[count + i], refs[2 * count].at[i]) for i in range(count)
    ]
    for copy in copies:
        copy.start()
    for copy in copies:
        copy.wait()


def fetch(*args):
    args = [pltpu.with_memory_space_constraint(a, pltpu.HBM) for a in args]
    return pl.pallas_call(
        functools.partial(fetch_kernel, len(args)),
        out_shape=[pltpu.VMEM(a.shape, a.dtype) for a in args],
        in_specs=[pl.BlockSpec(memory_space=pltpu.HBM)] * len(args),
        out_specs=[pl.BlockSpec(memory_space=pltpu.VMEM)] * len(args),
        scratch_shapes=[pltpu.SemaphoreType.DMA((len(args),))],
        compiler_params=pltpu.CompilerParams(vmem_limit_bytes=2**20),
        cost_estimate=pl.CostEstimate(flops=10**9, bytes_accessed=9 * 2**20, transcendentals=0),
        name="fetch",
    )(*args)


def run_cell(blocks, heads, *args):
    own, f32 = blocks[0].shape[0], jnp.float32
    args = [pltpu.with_memory_space_constraint(a, pltpu.VMEM) for a in args]
    shapes = [
        ((own, heads * DV), jnp.bfloat16),
        ((own, heads, DK), f32),
        ((heads, own), f32),
        ((own, heads), f32),
        ((own, heads), f32),
        ((own, heads * DK), jnp.bfloat16),
        ((own, heads * DV), jnp.bfloat16),
    ]
    in_vmem = pl.BlockSpec(memory_space=pltpu.VMEM)
    return pl.pallas_call(
        functools.partial(cell_kernel, heads),
        out_shape=[jax.ShapeDtypeStruct(*s) for s in shapes],
        in_specs=[in_vmem] * (len(blocks) + len(args)),
        out_specs=[in_vmem] * len(shapes),
        compiler_params=pltpu.CompilerParams(vmem_limit_bytes=8 * 2**20),
        cost_estimate=pl.CostEstimate(flops=10**9, bytes_accessed=9 * 2**20, transcendentals=0),
        name="cell",
    )(*blocks, *args)


STEP = 4
EARLY = 4


def update_rows(rows, memory_ref, keep_ref, admit_ref, keys_ref, values_ref, staged_ref, emit):
    f32 = jnp.float32
    count, heads = keep_ref.shape
    values = values_ref[...].astype(f32)
    values = jnp.concatenate([values, jnp.zeros((128 - count, values.shape[1]), f32)], axis=0)
    columns = [jnp.transpose(values[:, h * DV : (h + 1) * DV]) for h in range(heads)]
    keys = keys_ref[...].astype(f32) * DK ** (-0.5)
    for n, r in enumerate(rows):
        if emit is not None and n % STEP == 0:
            emit("need", n)
        for h in range(heads):
            key = keys[r : r + 1, h * DK : (h + 1) * DK] * admit_ref[r : r + 1, h : h + 1]
            added = columns[h][:, r : r + 1] * key
            staged_ref[n, h] = keep_ref[r : r + 1, h : h + 1] * memory_ref[n, h] + added
        if n % STEP == STEP - 1:
            emit("done", n)


def update_kernel(rows, early, count, *refs):
    if early:
        memory_ref, *small = refs[:5]
        given, refs = refs[5 : 5 + count], refs[5 + count :]
        out_ref, held_refs, refs = refs[0], refs[1 : 1 + count], refs[1 + count :]
        staged_ref, sems, held_sems = refs
    else:
        memory_hbm, *small = refs[1:6]
        given, refs = refs[6 : 6 + count], refs[6 + count :]
        out_ref, held_refs, refs = refs[0], refs[1 : 1 + count], refs[1 + count :]
        staged_ref, sems, held_sems, memory_ref, in_sems = refs
    parts = [pl.ds(n, STEP) for n in range(0, len(rows), STEP)]
    places = [pl.ds(rows[n], STEP) for n in range(0, len(rows), STEP)]
    outward = [
        pltpu.make_async_copy(staged_ref.at[p], out_ref.at[q], sems.at[n])
        for n, (p, q) in enumerate(zip(parts, places))
    ]
    inward = []
    if not early:
        inward = [
            pltpu.make_async_copy(memory_hbm.at[q], memory_ref.at[p], in_sems.at[n])
            for n, (p, q) in enumerate(zip(parts, places))
        ]
    held = [
        pltpu.make_async_copy(a, b, held_sems.at[n])
        for n, (a, b) in enumerate(zip(given, held_refs))
    ]
    for copy in inward + held:
        copy.start()

    def emit(what, n):
        if what == "need" and inward:
            inward[n // STEP].wait()
        if what == "done":
            outward[n // STEP].start()

    update_rows(rows, memory_ref, *small, staged_ref, emit)
    for copy in outward + held:
        copy.wait()


def run_update(memory, small, weights, before=None, rows=()):
    vmem, hbm = pl.BlockSpec(memory_space=pltpu.VMEM), pl.BlockSpec(memory_space=pltpu.HBM)
    early = before is None
    staged = pltpu.VMEM((len(rows),) + memory.shape[1:], memory.dtype)
    sems = pltpu.SemaphoreType.DMA((len(rows) // STEP,))
    scratch = [staged, sems, pltpu.SemaphoreType.DMA((len(weights),))]
    if early:
        args = [pltpu.with_memory_space_constraint(a, pltpu.VMEM) for a in (memory, *small)]
        in_specs = [vmem] * len(args)
    else:
        args = [pltpu.with_memory_space_constraint(a, pltpu.HBM) for a in (before, memory)]
        args += list(small)
        in_specs = [hbm] * 2 + [vmem] * len(small)
        scratch += [staged, sems]
    args += [pltpu.with_memory_space_constraint(w, pltpu.HBM) for w in weights]
    return pl.pallas_call(
        functools.partial(update_kernel, rows, early, len(weights)),
        out_shape=[pltpu.HBM(memory.shape, memory.dtype)]
        + [pltpu.VMEM(w.shape, w.dtype) for w in weights],
        in_specs=in_specs + [hbm] * len(weights),
        out_specs=[hbm] + [vmem] * len(weights),
        scratch_shapes=scratch,
        input_output_aliases={} if early else {0: 0},
        compiler_params=pltpu.CompilerParams(vmem_limit_bytes=12 * 2**20),
        cost_estimate=pl.CostEstimate(flops=10**9, bytes_accessed=9 * 2**20, transcendentals=0),
        name="update" if early else "update_rest",
    )(*args)


def second_kernel(*refs):
    blocks = lax.axis_size("tp")
    projs, tokens = refs[blocks : blocks + 2], refs[blocks + 2 : blocks + 4]
    sent_ref, second_ref, square_ref = refs[blocks + 4 :]
    f32 = jnp.float32
    me = lax.axis_index("tp")
    part = second_ref.shape[0]
    rows = pl.ds(pl.multiple_of((me & 1) * part, part), part)
    width, columns = refs[0].shape[1], tokens[0].shape[1]
    square = 0.0
    for n in range(2):
        total = tokens[n][rows, :].astype(f32)
        for b in range(blocks):
            at = pl.ds(pl.multiple_of((me ^ b) * width, width), width)
            total += jnp.dot(refs[b][rows, :], projs[n][at, :], preferred_element_type=f32)
        second = total.astype(jnp.bfloat16)
        cols = slice(n * columns, (n + 1) * columns)
        second_ref[:, cols] = second
        for i in range(sent_ref.shape[0]):
            sent_ref[i, :, cols] = second
        second = second.astype(f32)
        square += jnp.sum(second * second, axis=1, keepdims=True)
    square_ref[...] = square


def up_kernel(rows_ref, gain_ref, gain_other_ref, up_ref, up_other_ref, out_ref):
    f32 = jnp.float32
    total = 0.0
    width = up_ref.shape[0]
    for n, (gain, up) in enumerate(((gain_ref, up_ref), (gain_other_ref, up_other_ref))):
        rows = rows_ref[:, :, n * width : (n + 1) * width].astype(f32) * gain[...]
        rows = rows.reshape(-1, width).astype(jnp.bfloat16)
        total += jnp.dot(rows, up[...], preferred_element_type=f32)
    out_ref[...] = total.astype(jnp.bfloat16)


def down_kernel(sent_ref, came_ref, down_ref, down_other_ref, out_ref):
    f32 = jnp.float32
    preact = sent_ref[...].astype(f32) + came_ref[...].astype(f32)
    hidden = jnp.square(jnp.maximum(preact, 0.0)).astype(jnp.bfloat16)
    width = down_ref.shape[1]
    for n, down in enumerate((down_ref, down_other_ref)):
        partial = jnp.dot(hidden, down[...], preferred_element_type=f32).astype(jnp.bfloat16)
        partial = partial.reshape(out_ref.shape[0], out_ref.shape[1], width)
        out_ref[:, :, n * width : (n + 1) * width] = partial


def run_plain(kernel, name, shapes, held, *args):
    in_vmem = pl.BlockSpec(memory_space=pltpu.VMEM)
    args = [
        pltpu.with_memory_space_constraint(a, pltpu.VMEM) if n < held else a
        for n, a in enumerate(args)
    ]
    return pl.pallas_call(
        kernel,
        out_shape=[jax.ShapeDtypeStruct(*s) for s in shapes],
        in_specs=[in_vmem] * len(args),
        out_specs=[in_vmem] * len(shapes),
        compiler_params=pltpu.CompilerParams(vmem_limit_bytes=8 * 2**20),
        cost_estimate=pl.CostEstimate(flops=10**9, bytes_accessed=2**21, transcendentals=0),
        name=name,
    )(*args)


def swap(array, bit):
    pairs = [(i, i ^ bit) for i in range(lax.axis_size("tp"))]
    return lax.ppermute(array, "tp", pairs)


def per_device(
    tokens,
    memory,
    normalizer,
    stabilizer,
    norm_gain,
    query_weight,
    key_weight,
    value_weight,
    outgate_weight,
    input_gate_weight,
    forget_gate_weight,
    forget_bias,
    memory_gain,
    proj_weight,
    ffn_gain,
    up_weight,
    down_weight,
):
    own_rows = tokens.shape[0]
    heads_here = memory.shape[1]
    blocks = [tokens] + [swap(tokens, b) for b in reversed(range(1, lax.axis_size("tp")))][::-1]
    held = fetch(
        norm_gain.reshape(1, -1),
        query_weight,
        key_weight,
        value_weight,
        outgate_weight,
        input_gate_weight.T,
        forget_gate_weight.T,
        forget_bias.reshape(1, -1),
        stabilizer.T,
        normalizer,
        memory,
        memory_gain.reshape(1, -1),
    )
    mixed, normalizer_new, stab_new, keep, admit, keys, values = run_cell(blocks, heads_here, *held)
    stab_new = stab_new.T
    kv, tp = lax.axis_size("kv"), lax.axis_size("tp")
    bf, f32 = jnp.bfloat16, jnp.float32
    mixed_blocks = [mixed] + [swap(mixed, b) for b in range(1, tp)]
    mixed, *given = lax.optimization_barrier(
        (mixed, proj_weight, ffn_gain.reshape(1, -1), up_weight)
    )
    proj_other, gain_other, up_other = (swap(w, 1) for w in given)
    up_other = pltpu.with_memory_space_constraint(up_other, pltpu.VMEM)
    small = (keep, admit, keys, values)
    begun = tuple(range(own_rows * EARLY // 8))
    memory_part, proj_held = run_update(held[10], small, (proj_weight,), rows=begun)
    part, columns = own_rows // 2, 2 * tokens.shape[1]
    shapes = [((kv, part, columns), bf), ((part, columns), bf), ((part, 1), f32)]
    sent, second, square_sum = run_plain(
        second_kernel, "second", shapes, tp + 4, *mixed_blocks, proj_held, proj_other, *blocks[:2]
    )
    sent, gain_other, up_other = lax.optimization_barrier((sent, gain_other, up_other))
    rows = lax.all_to_all(sent, "kv", 0, 0, tiled=True)
    gains = (ffn_gain.reshape(1, -1), gain_other)
    shapes = [((kv * part, up_weight.shape[1]), bf)]
    (sent,) = run_plain(up_kernel, "up", shapes, 0, rows, *gains, up_weight, up_other)
    sent, small, square_sum, down_weight = lax.optimization_barrier(
        (sent, small, square_sum, down_weight)
    )
    down_other = swap(down_weight, 1)
    memory_new, down_held = run_update(
        memory,
        small,
        (down_weight,),
        before=memory_part,
        rows=tuple(range(len(begun), own_rows)),
    )
    bit = 2
    while bit < tp:
        if bit > 2:
            sent = (sent.astype(f32) + came.astype(f32)).astype(bf)
        came = swap(sent, bit)
        square_sum = square_sum + swap(square_sum, bit)
        bit *= 2
    scale_two = lax.rsqrt(square_sum / D + EPS)
    factor = jnp.broadcast_to(scale_two * scale_two, second.shape)
    came, memory_new, factor, second = lax.optimization_barrier((came, memory_new, factor, second))
    shapes = [((kv, part, columns), bf)]
    (sent,) = run_plain(
        down_kernel, "down", shapes, 0, sent, came, down_held, down_other
    )
    got = lax.all_to_all(sent, "kv", 0, 0, tiled=True)
    summed = jnp.sum(got.astype(f32), axis=0)
    done = (second.astype(f32) + summed * factor).astype(bf)
    kept, given = jnp.split(done, 2, axis=1)
    taken = swap(given, 1)
    first = (lax.axis_index("tp") & 1) == 0
    layer_out = jnp.concatenate(
        [jnp.where(first, kept, taken), jnp.where(first, taken, kept)], axis=0
    )
    return (layer_out, memory_new, normalizer_new, stab_new)


def solution(mesh):
    placed = (
        P("kv", "tp"),
        P("kv", "tp", None, None),
        P("kv", "tp", None),
        P("kv", "tp"),
        P(),
        P(None, "tp"),
        P(None, "tp"),
        P(None, "tp"),
        P(None, "tp"),
        P(),
        P(),
        P(),
        P("tp"),
        P(None, "tp"),
        P("tp"),
        P("tp", "kv"),
        P("kv", "tp"),
    )
    return jax.shard_map(
        per_device,
        mesh=mesh,
        in_specs=placed,
        out_specs=(P("kv", "tp"), P("kv", "tp", None, None), P("kv", "tp", None), P("kv", "tp")),
        check_vma=False,
    )
```
